32 devices in a mesh: grp: 2 (over y), ep: 4 (over z), tp: 4 (over x, core).
Axes of the slice: x: 2, y: 2, z: 4, core: 2. Of those that a mesh axis runs over, the one named last changes fastest.
Arguments:
- conv_input: bfloat16 [5120, 2048], P(('grp', 'ep')), parts along dimension 0, may hold values from -6 to 6
- conv_taps: float32 [31, 2048], replicated, may hold values from -1 to 1
- conv_gain: float32 [2048], replicated, may hold values from 0.1 to 1.9
- conv_weight: bfloat16 [2048, 2048], P(None, 'tp'), may hold values from -0.125 to 0.125
- moe_input: bfloat16 [5120, 2048], P(('grp', 'ep')), parts along dimension 0, may hold values from -6 to 6
- moe_gain: float32 [2048], replicated, may hold values from 0.1 to 1.9
- expert_ids: int32 [5120, 2], P(('grp', 'ep')), parts along dimension 0, may hold values from 0 to 3, as said below
- route_weights: float32 [5120, 2], P(('grp', 'ep')), parts along dimension 0, may hold values from 0.1 to 1
- gate_weight: bfloat16 [4, 2048, 1024], P('ep', None, 'tp'), may hold values from -0.125 to 0.125
- up_weight: bfloat16 [4, 2048, 1024], P('ep', None, 'tp'), may hold values from -0.125 to 0.125
- down_weight: bfloat16 [4, 1024, 2048], P('ep', 'tp'), may hold values from -0.1875 to 0.1875
- post_gain: float32 [2048], replicated, may hold values from 0.1 to 1.9
Outputs:
- conv_out: bfloat16 [5120, 2048], P(('grp', 'ep'), 'tp'), parts along dimension 0
- moe_out: bfloat16 [5120, 2048], P(('grp', 'ep', 'tp')), parts along dimension 0
The draws below stay inside these ranges and needn't reach their ends.
There are 2 independent parts, one for each index of `grp`. The reference program is written for one: setup_inputs(seed, part) draws one part's arguments, and reference() takes and returns one part's arrays. A program takes and returns all parts, laid end to end along the dimension named above; an argument that names none is the same for every part. Nothing has to cross between parts.
Inputs may be any that keep to these rules, and one draw needn't show every extreme that they name: `expert_ids`: in each aligned block of 160 tokens, every expert is named exactly 80 times; a token's two experts differ and lie in one group of 4 consecutive experts.
All inputs are finite; a program needn't handle non-finite values.
Results may differ from the reference program's by a relative error of at most 0.012.
Values may be sent and summed in bfloat16 or wider, within the bound.
A program may use at most 128 MiB of HBM per device.

```python
import jax
import jax.numpy as jnp
from jax import lax

D = 2048
FF = 1024
KW = 31
GROUP = 4
TOPK = 2
EXPERTS = 4
TOKENS = 2560
BLOCK = 160
N_TP = 4


def draw_expert_ids(key, part):
    block_count = TOKENS // BLOCK
    key_list = jax.random.split(jax.random.fold_in(key, 7), block_count)

    def one_block(block_key):
        key_perm, key_shift = jax.random.split(block_key)
        ordering = jax.random.permutation(key_perm, BLOCK)
        offset = jax.random.randint(key_shift, (), 0, GROUP - 1)
        primary = ordering % EXPERTS
        second = primary // GROUP * GROUP + (primary % GROUP + 1 + offset) % GROUP
        return jnp.stack([primary, second], axis=1)
    return jax.vmap(one_block)(key_list).reshape(TOKENS, 2).astype(jnp.int32)


def shard_levels(own_key, extent, cuts, low, high):
    level = 1.0
    for dim, parts in cuts:
        draws = jax.random.uniform(jax.random.fold_in(jax.random.fold_in(own_key, 6), dim), (parts,), jnp.float32, low / len(cuts), high / len(cuts))
        level = level * jnp.repeat(jnp.exp(draws), extent[dim] // parts).reshape((-1,) + (1,) * (len(extent) - 1 - dim))
    return level


def bell_draw(key, shape, scale, limit, cuts=(), kind=jnp.bfloat16):
    result = jax.random.normal(key, shape, jnp.float32) * scale
    if len(cuts) > 0:
        result = shard_levels(key, shape, cuts, -0.22, 0.18) * result
    return jnp.clip(result, min=-limit, max=limit).astype(kind)


def setup_inputs(seed: int = 0, part: int = 0) -> dict:
    keys = jax.random.split(jax.random.key(seed), 13)
    part_splits = jax.random.split(jax.random.fold_in(keys[12], part), 13)
    conv_input = bell_draw(part_splits[0], (TOKENS, D), 1.0, 6.0, ((0, 4),))
    conv_taps = bell_draw(keys[1], (KW, D), KW ** -0.5, 1.0, (), jnp.float32)
    conv_gain = jnp.clip(1.0 + 0.18 * jax.random.normal(keys[2], (D,), jnp.float32), 0.1, 1.9)
    conv_weight = bell_draw(keys[3], (D, D), D ** -0.5, 0.125, ((1, 4),))
    moe_input = bell_draw(part_splits[4], (TOKENS, D), 1.0, 6.0, ((0, 4),))
    moe_gain = jnp.clip(1.0 + 0.18 * jax.random.normal(keys[5], (D,), jnp.float32), 0.1, 1.9)
    expert_ids = draw_expert_ids(jax.random.fold_in(jax.random.fold_in(keys[12], part), 71), part)
    route_weights = jnp.clip(0.1 + 0.9 * jax.random.uniform(part_splits[7], (TOKENS, TOPK), jnp.float32) ** shard_levels(part_splits[7], (TOKENS, TOPK), ((0, 4),), -0.2, 0.2), 0.1, 1.0)
    gate_weight = bell_draw(keys[8], (EXPERTS, D, FF), D ** -0.5, 0.125, ((0, 4), (2, 4)))
    up_weight = bell_draw(keys[9], (EXPERTS, D, FF), D ** -0.5, 0.125, ((0, 4), (2, 4)))
    down_weight = bell_draw(keys[10], (EXPERTS, FF, D), FF ** -0.5, 0.1875, ((0, 4), (1, 4)))
    post_gain = jnp.clip(1.0 + 0.18 * jax.random.normal(keys[11], (D,), jnp.float32), 0.1, 1.9)
    return dict(conv_input=conv_input, conv_taps=conv_taps, conv_gain=conv_gain, conv_weight=conv_weight, moe_input=moe_input, moe_gain=moe_gain, expert_ids=expert_ids, route_weights=route_weights, gate_weight=gate_weight, up_weight=up_weight, down_weight=down_weight, post_gain=post_gain)


EPSILON = 1e-06

def channel_norm(values, scales):
    mean_square = lax.optimization_barrier(jnp.mean(values * values, axis=-1, keepdims=True))
    return values * lax.rsqrt(mean_square + EPSILON) * scales

def causal_conv(signal, kernel_taps):
    length = signal.shape[0]
    padded = jnp.pad(signal.astype(jnp.float32), ((KW - 1, 0), (0, 0)))
    conv_sum = jnp.zeros((length, signal.shape[1]), jnp.float32)
    for offset in range(KW):
        conv_sum = conv_sum + padded[offset:offset + length] * kernel_taps[offset]
    return conv_sum

def expert_apply(operands):
    expert_rows, gate_part, up_part, down_part = operands
    gate_value = jnp.dot(expert_rows, gate_part, preferred_element_type=jnp.float32)
    up_value = jnp.dot(expert_rows, up_part, preferred_element_type=jnp.float32)
    hidden = (jax.nn.silu(gate_value) * up_value).astype(jnp.bfloat16)
    pieces = hidden.reshape(hidden.shape[0], N_TP, FF // N_TP).astype(jnp.float32)
    down_pieces = down_part.reshape(N_TP, FF // N_TP, D).astype(jnp.float32)
    partial_value = jnp.einsum('ctf,tfd->tcd', pieces, down_pieces)
    partial_value = lax.optimization_barrier(partial_value.astype(jnp.bfloat16)).astype(jnp.float32)
    return lax.optimization_barrier(jnp.sum(partial_value, axis=0)).astype(jnp.bfloat16)

def reference(conv_input, conv_taps, conv_gain, conv_weight, moe_input, moe_gain, expert_ids, route_weights, gate_weight, up_weight, down_weight, post_gain):
    conv_sum = causal_conv(conv_input, conv_taps)
    activated = jax.nn.silu(channel_norm(conv_sum, conv_gain)).astype(jnp.bfloat16)
    conv_out = jnp.dot(activated, conv_weight, preferred_element_type=jnp.float32).astype(jnp.bfloat16)
    normed = channel_norm(moe_input.astype(jnp.float32), moe_gain).astype(jnp.bfloat16)
    flat_ids = expert_ids.reshape(-1).astype(jnp.int32)
    entry_count = flat_ids.shape[0]
    per_expert = entry_count // EXPERTS
    onehot = (flat_ids[:, None] == jnp.arange(EXPERTS, dtype=jnp.int32)[None, :]).astype(jnp.int32)
    position = lax.optimization_barrier(jnp.sum((jnp.cumsum(onehot, axis=0) - 1) * onehot, axis=1)).astype(jnp.int32)
    target = (flat_ids * per_expert + position).astype(jnp.int32)
    source_entry = jnp.zeros((entry_count,), jnp.int32).at[target].set(jnp.arange(entry_count, dtype=jnp.int32))
    expert_rows = normed[source_entry // 2].reshape(EXPERTS, per_expert, D)
    results = lax.map(expert_apply, (expert_rows, gate_weight, up_weight, down_weight))
    entry_results = results.reshape(entry_count, D)[target].reshape(-1, TOPK, D).astype(jnp.float32)
    mixed_rows = lax.optimization_barrier(jnp.sum(entry_results * route_weights[:, :, None], axis=1))
    moe_out = channel_norm(mixed_rows, post_gain).astype(jnp.bfloat16)
    return (conv_out, moe_out)
```

```python
import functools

import jax
import jax.numpy as jnp
from jax import lax
from jax.experimental import pallas as pl
from jax.experimental.pallas import tpu as pltpu
from jax.sharding import PartitionSpec as P

EPSILON = 1e-06
MESH = pl.DeviceIdType.MESH
F32, BF16 = jnp.float32, jnp.bfloat16
CONV_ROWS = 64
LANES = 128


def silu(v):
    return v / (1.0 + jnp.exp(-v))


def kernel(
    sizes,
    conv_hbm,
    taps,
    conv_gain,
    convw_hbm,
    moe_hbm,
    moe_gain,
    ids_ref,
    route_ref,
    gate_hbm,
    up_hbm,
    down_hbm,
    post_gain,
    conv_out,
    moe_out,
    ext,
    convw,
    act,
    conv_sum,
    own_in,
    gate,
    up,
    down,
    mix,
    send_rows,
    got_rows,
    gate_val,
    hidden,
    result,
    back,
    sem_local,
    sem_halo,
    sem_a,
    sem_b,
    sem_c,
    sem_d,
    sem_e,
    sem_x,
    sem_y,
):
    groups, eps, tps = sizes
    highs = tps // 2
    g, e, t = lax.axis_index("grp"), lax.axis_index("ep"), lax.axis_index("tp")
    hi, lo = t // 2, t % 2
    partner = hi * 2 + (1 - lo)
    rows = conv_hbm.shape[0]
    width = conv_hbm.shape[1]
    reach = taps.shape[0] - 1
    halo = ext.shape[0] - rows
    block = own_in.shape[0]
    slots = 2 * block
    cap = slots // eps
    units = gate.shape[2]

    local = [
        pltpu.make_async_copy(
            moe_hbm.at[pl.ds(pl.multiple_of(t * block, 16), block)], own_in, sem_local.at[0]
        ),
        pltpu.make_async_copy(conv_hbm, ext.at[pl.ds(halo, rows)], sem_local.at[1]),
        pltpu.make_async_copy(convw_hbm, convw, sem_local.at[2]),
        pltpu.make_async_copy(gate_hbm.at[0], gate.at[t], sem_local.at[3]),
        pltpu.make_async_copy(up_hbm.at[0], up.at[t], sem_local.at[4]),
        pltpu.make_async_copy(down_hbm.at[0], down.at[t], sem_local.at[5]),
    ]
    for copy in local:
        copy.start()

    barrier = pltpu.get_barrier_semaphore()
    greet = [{"tp": partner}]
    greet += [{"tp": (hi + dh) % highs * 2 + lo} for dh in range(1, highs)]
    greet += [{"grp": (g + dg) % groups} for dg in range(1, groups)]
    greet += [{"ep": (e + de) % eps} for de in range(1, eps)]
    for other in greet:
        pl.semaphore_signal(barrier, inc=1, device_id=other, device_id_type=MESH)
    pl.semaphore_wait(barrier, len(greet))

    def remote(src, dst, sems, index, device):
        return pltpu.make_async_remote_copy(
            src_ref=src,
            dst_ref=dst,
            send_sem=sems.at[(0,) + index],
            recv_sem=sems.at[(1,) + index],
            device_id=device,
            device_id_type=MESH,
        )

    items = []
    half = width // 2
    for source, buffer in ((gate_hbm, gate), (up_hbm, up)):
        for part in range(2):
            items.append((source, buffer, part * half, half, 0, units))
    for part in range(2):
        items.append((down_hbm, down, 0, units, part * half, half))

    def view(ref, item, piece=None):
        _, _, r0, count, c0, columns = item
        if piece is None:
            return ref.at[pl.ds(r0, count), pl.ds(c0, columns)]
        size = count // groups
        start = pl.multiple_of(r0 + piece * size, 16)
        return ref.at[pl.ds(start, size), pl.ds(c0, columns)]

    def copy_a(i):
        item = items[i]
        return remote(
            view(item[0].at[0], item), view(item[1].at[t], item), sem_a, (i,), {"tp": partner}
        )

    def copy_b(i, dh):
        item = items[i]
        other = (hi + dh) % highs * 2 + lo
        return remote(
            view(item[0].at[0], item, g), view(item[1].at[t], item, g), sem_b, (i, dh), {"tp": other}
        )

    def origin(dh):
        return (hi + highs - dh) % highs * 2 + lo

    def copy_c(i, dh, dg):
        item = items[i]
        ref = view(item[1].at[origin(dh)], item, g)
        return remote(ref, ref, sem_c, (i, dh, dg), {"grp": (g + dg) % groups})

    def copy_d(i, dh):
        item = items[i]
        ref = view(item[1].at[origin(dh)], item, g)
        return remote(ref, ref, sem_d, (i, dh), {"tp": partner})

    def copy_e(i, dh, dg):
        item = items[i]
        ref = view(item[1].at[origin(dh)], item, (g + groups - dg) % groups)
        return remote(ref, ref, sem_e, (i, dh, dg), {"tp": partner})

    count = len(items)
    for i in range(count):
        for dh in range(1, highs):
            copy_b(i, dh).start()
    for i in range(count):
        copy_a(i).start()

    def relay_cross(i):
        for dh in range(1, highs):
            copy_b(i, dh).wait_recv()
            for dg in range(1, groups):
                copy_c(i, dh, dg).start()
            copy_d(i, dh).start()

    def relay_group(i):
        for dh in range(1, highs):
            for dg in range(1, groups):
                copy_c(i, dh, dg).wait_recv()
                copy_e(i, dh, dg).start()

    def arrived(i):
        copy_a(i).wait_recv()
        for dh in range(1, highs):
            copy_d(i, dh).wait_recv()
            for dg in range(1, groups):
                copy_e(i, dh, dg).wait_recv()

    halo_copy = remote(
        conv_hbm.at[pl.ds(rows - halo, halo)],
        ext.at[pl.ds(0, halo)],
        sem_halo,
        (0,),
        {"ep": (e + 1) % eps},
    )

    @pl.when(e < eps - 1)
    def _():
        halo_copy.start()

    @pl.when(e == 0)
    def _():
        ext[0:halo, :] = jnp.zeros((halo, width), BF16)

    ids = ids_ref[pl.ds(pl.multiple_of(t * block, 8), block), :]
    weights = route_ref[pl.ds(pl.multiple_of(t * block, 8), block), :]
    lane = lax.broadcasted_iota(jnp.int32, (block, LANES), 1)
    below = (
        lax.broadcasted_iota(jnp.int32, (block, block), 0)
        > lax.broadcasted_iota(jnp.int32, (block, block), 1)
    )
    below = jnp.where(below, 1.0, 0.0).astype(BF16)
    slot = lax.broadcasted_iota(jnp.int32, (block, slots), 1).astype(F32)
    seen = jnp.zeros((1, LANES), F32)
    pick = jnp.zeros((block, slots), F32)
    mixing = jnp.zeros((block, slots), F32)
    for k in range(2):
        named = ids[:, k : k + 1]
        onehot = jnp.where(named == lane, 1.0, 0.0)
        before = jnp.dot(below, onehot.astype(BF16), preferred_element_type=F32) + seen
        position = jnp.sum(before * onehot, axis=1, keepdims=True)
        seen = seen + jnp.sum(onehot, axis=0, keepdims=True)
        target = named.astype(F32) * float(cap) + position
        here = jnp.where(target == slot, 1.0, 0.0)
        pick = pick + here
        mixing = mixing + here * weights[:, k : k + 1]
    mix_high = mixing.astype(BF16)
    mix[0] = mix_high
    mix[1] = (mixing - mix_high.astype(F32)).astype(BF16)

    local[0].wait()
    own = own_in[...].astype(F32)
    scale = lax.rsqrt(jnp.mean(own * own, axis=1, keepdims=True) + EPSILON)
    normed = (own * scale * moe_gain[...]).astype(BF16)
    chosen = lax.dot_general(
        pick.astype(BF16), normed, (((0,), (0,)), ((), ())), preferred_element_type=F32
    ).astype(BF16)
    send_rows[...] = chosen.reshape(eps, cap, width)

    def copy_x(de):
        other = (e + de) % eps
        return remote(send_rows.at[other], got_rows.at[e], sem_x, (de,), {"ep": other})

    def copy_y(de, part):
        other = (e + de) % eps
        columns = pl.ds(part * half, half)
        return remote(
            result.at[other, :, columns],
            back.at[e, :, columns],
            sem_y,
            (de, part),
            {"ep": other},
        )

    for de in range(1, eps):
        copy_x(de).start()
    got_rows[pl.ds(e, 1)] = send_rows[pl.ds(e, 1)]

    local[1].wait()

    def conv_chunk(j):
        row0 = pl.multiple_of(j * CONV_ROWS, CONV_ROWS)
        tall = CONV_ROWS + halo

        def columns_of(c):
            return pl.ds(pl.multiple_of(c * LANES, LANES), LANES)

        def first(c, squares):
            columns = columns_of(c)
            window = ext[pl.ds(row0, tall), columns].astype(F32)
            total = jnp.zeros((CONV_ROWS, LANES), F32)
            for phase in range(8):
                shifts = [k for k in range(halo - reach, halo + 1) if k % 8 == phase]
                top = max(shifts) - phase
                shifted = window[phase : phase + top + CONV_ROWS]
                for k in shifts:
                    tap = taps[pl.ds(k - halo + reach, 1), columns]
                    total = total + shifted[k - phase : k - phase + CONV_ROWS] * tap
            conv_sum[:, columns] = total
            return squares + total * total

        squares = lax.fori_loop(0, width // LANES, first, jnp.zeros((CONV_ROWS, LANES), F32))
        mean = jnp.sum(squares, axis=1, keepdims=True) * (1.0 / width)
        rate = lax.rsqrt(mean + EPSILON)

        def second(c, carry):
            columns = columns_of(c)
            value = conv_sum[:, columns] * rate * conv_gain[:, columns]
            act[pl.ds(row0, CONV_ROWS), columns] = silu(value).astype(BF16)
            return carry

        lax.fori_loop(0, width // LANES, second, 0)

    chunks = rows // CONV_ROWS

    def conv_range(start, stop):
        def step(j, carry):
            conv_chunk(j)
            return carry

        lax.fori_loop(start, stop, step, 0)

    cuts = [1 + (chunks - 1) * i // 4 for i in range(5)]
    conv_range(cuts[0], cuts[1])
    relay_cross(0)
    conv_range(cuts[1], cuts[2])
    relay_cross(1)
    relay_group(0)
    conv_range(cuts[2], cuts[3])
    relay_cross(2)
    relay_group(1)
    conv_range(cuts[3], cuts[4])

    @pl.when(e > 0)
    def _():
        halo_copy.wait_recv()

    conv_range(0, 1)
    relay_cross(3)
    relay_group(2)

    local[2].wait()
    out_rows = rows // 2

    def project(j, carry):
        where = pl.ds(pl.multiple_of(j * out_rows, 16), out_rows)
        conv_out[where, :] = jnp.dot(
            act[where, :], convw[...], preferred_element_type=F32
        ).astype(BF16)
        return carry

    lax.fori_loop(0, 2, project, 0)

    relay_cross(4)
    relay_group(3)
    for de in range(1, eps):
        copy_x(de).wait_recv()
    local[3].wait()
    arrived(0)
    arrived(1)

    def gates(q, carry):
        gate_val[q] = jnp.dot(
            got_rows[...].reshape(slots, width), gate[q], preferred_element_type=F32
        )
        return carry

    lax.fori_loop(0, tps, gates, 0)
    relay_cross(5)
    relay_group(4)
    local[4].wait()
    arrived(2)
    arrived(3)

    def ups(q, carry):
        value = jnp.dot(got_rows[...].reshape(slots, width), up[q], preferred_element_type=F32)
        hidden[q] = (silu(gate_val[q]) * value).astype(BF16)
        return carry

    lax.fori_loop(0, tps, ups, 0)
    local[5].wait()
    tile = 256
    for part in range(2):
        if part == 1:
            relay_group(5)
        arrived(4 + part)

        def downs(n, carry):
            columns = pl.ds(pl.multiple_of(part * half + n * tile, tile), tile)
            value = jnp.dot(hidden[0], down[0, :, columns], preferred_element_type=F32)
            for q in range(1, tps):
                value = value + jnp.dot(hidden[q], down[q, :, columns], preferred_element_type=F32)
            result[:, :, columns] = value.astype(BF16).reshape(eps, cap, tile)
            return carry

        lax.fori_loop(0, half // tile, downs, 0)
        for de in range(1, eps):
            copy_y(de, part).start()
    back[pl.ds(e, 1)] = result[pl.ds(e, 1)]
    for de in range(1, eps):
        for part in range(2):
            copy_y(de, part).wait_recv()
    every = back[...].reshape(slots, width)
    mixed = jnp.dot(mix[0], every, preferred_element_type=F32) + jnp.dot(
        mix[1], every, preferred_element_type=F32
    )
    scale = lax.rsqrt(jnp.mean(mixed * mixed, axis=1, keepdims=True) + EPSILON)
    moe_out[...] = (mixed * scale * post_gain[...]).astype(BF16)

    @pl.when(e < eps - 1)
    def _():
        halo_copy.wait_send()

    for i in range(count):
        copy_a(i).wait_send()
        for dh in range(1, highs):
            copy_b(i, dh).wait_send()
            copy_d(i, dh).wait_send()
            for dg in range(1, groups):
                copy_c(i, dh, dg).wait_send()
                copy_e(i, dh, dg).wait_send()
    for de in range(1, eps):
        copy_x(de).wait_send()
        for part in range(2):
            copy_y(de, part).wait_send()


def body(
    sizes,
    conv_input,
    conv_taps,
    conv_gain,
    conv_weight,
    moe_input,
    moe_gain,
    expert_ids,
    route_weights,
    gate_weight,
    up_weight,
    down_weight,
    post_gain,
):
    groups, eps, tps = sizes
    highs = tps // 2
    rows, width = conv_input.shape
    block = moe_input.shape[0] // tps
    cap = 2 * block // eps
    units = gate_weight.shape[2]
    halo = (conv_taps.shape[0] - 1 + 15) // 16 * 16
    vmem = pl.BlockSpec(memory_space=pltpu.VMEM)
    hbm = pl.BlockSpec(memory_space=pl.ANY)
    dma = pltpu.SemaphoreType.DMA
    items = 6
    call = pl.pallas_call(
        functools.partial(kernel, sizes),
        out_shape=(
            jax.ShapeDtypeStruct((rows, conv_weight.shape[1]), BF16),
            jax.ShapeDtypeStruct((block, width), BF16),
        ),
        in_specs=[hbm, vmem, vmem, hbm, hbm, vmem, vmem, vmem, hbm, hbm, hbm, vmem],
        out_specs=(vmem, vmem),
        scratch_shapes=[
            pltpu.VMEM((rows + halo, width), BF16),
            pltpu.VMEM(conv_weight.shape, BF16),
            pltpu.VMEM((rows, width), BF16),
            pltpu.VMEM((CONV_ROWS, width), F32),
            pltpu.VMEM((block, width), BF16),
            pltpu.VMEM((tps, width, units), BF16),
            pltpu.VMEM((tps, width, units), BF16),
            pltpu.VMEM((tps, units, width), BF16),
            pltpu.VMEM((2, block, 2 * block), BF16),
            pltpu.VMEM((eps, cap, width), BF16),
            pltpu.VMEM((eps, cap, width), BF16),
            pltpu.VMEM((tps, 2 * block, units), F32),
            pltpu.VMEM((tps, 2 * block, units), BF16),
            pltpu.VMEM((eps, cap, width), BF16),
            pltpu.VMEM((eps, cap, width), BF16),
            dma((6,)),
            dma((2, 1)),
            dma((2, items)),
            dma((2, items, highs)),
            dma((2, items, highs, groups)),
            dma((2, items, highs)),
            dma((2, items, highs, groups)),
            dma((2, eps)),
            dma((2, eps, 2)),
        ],
        compiler_params=pltpu.CompilerParams(
            collective_id=0, has_side_effects=True, vmem_limit_bytes=60 * 1024 * 1024
        ),
    )
    return call(
        conv_input,
        conv_taps,
        conv_gain.reshape(1, width),
        conv_weight,
        moe_input,
        moe_gain.reshape(1, width),
        expert_ids,
        route_weights,
        gate_weight,
        up_weight,
        down_weight,
        post_gain.reshape(1, width),
    )


def solution(mesh):
    in_specs = (
        P(("grp", "ep"), None),
        P(),
        P(),
        P(None, "tp"),
        P(("grp", "ep"), None),
        P(),
        P(("grp", "ep"), None),
        P(("grp", "ep"), None),
        P("ep", None, "tp"),
        P("ep", None, "tp"),
        P("ep", "tp", None),
        P(),
    )
    out_specs = (P(("grp", "ep"), "tp"), P(("grp", "ep", "tp"), None))
    sizes = (mesh.shape["grp"], mesh.shape["ep"], mesh.shape["tp"])
    return jax.shard_map(
        functools.partial(body, sizes),
        mesh=mesh,
        in_specs=in_specs,
        out_specs=out_specs,
        check_vma=False,
    )
```

```python
import functools

import jax
import jax.numpy as jnp
from jax import lax
from jax.experimental import pallas as pl
from jax.experimental.pallas import tpu as pltpu
from jax.sharding import PartitionSpec as P

EPSILON = 1e-06
MESH = pl.DeviceIdType.MESH
F32, BF16 = jnp.float32, jnp.bfloat16
CONV_ROWS = 64
LANES = 128
EARLY = 7


def silu(v):
    return v / (1.0 + jnp.exp(-v))


def kernel(
    sizes,
    conv_hbm,
    taps,
    conv_gain,
    convw_hbm,
    moe_hbm,
    moe_gain,
    ids_ref,
    route_ref,
    gate_hbm,
    up_hbm,
    down_hbm,
    post_gain,
    conv_out,
    moe_out,
    ext,
    convw,
    act,
    conv_sum,
    own_in,
    gate,
    up,
    down,
    mix,
    send_rows,
    got_rows,
    gate_val,
    hidden,
    result,
    back,
    sem_local,
    sem_halo,
    sem_a,
    sem_b,
    sem_c,
    sem_d,
    sem_e,
    sem_x,
    sem_y,
):
    groups, eps, tps = sizes
    highs = tps // 2
    g, e, t = lax.axis_index("grp"), lax.axis_index("ep"), lax.axis_index("tp")
    hi, lo = t // 2, t % 2
    partner = hi * 2 + (1 - lo)
    rows = conv_hbm.shape[0]
    width = conv_hbm.shape[1]
    reach = taps.shape[0] - 1
    halo = ext.shape[0] - rows
    block = own_in.shape[0]
    slots = 2 * block
    cap = slots // eps
    units = gate.shape[2]

    local = [
        pltpu.make_async_copy(
            moe_hbm.at[pl.ds(pl.multiple_of(t * block, 16), block)], own_in, sem_local.at[0]
        ),
        pltpu.make_async_copy(conv_hbm, ext.at[pl.ds(halo, rows)], sem_local.at[1]),
        pltpu.make_async_copy(convw_hbm, convw, sem_local.at[2]),
        pltpu.make_async_copy(gate_hbm.at[0], gate.at[t], sem_local.at[3]),
        pltpu.make_async_copy(up_hbm.at[0], up.at[t], sem_local.at[4]),
        pltpu.make_async_copy(down_hbm.at[0], down.at[t], sem_local.at[5]),
    ]
    for copy in local:
        copy.start()

    barrier = pltpu.get_barrier_semaphore()
    greet = [{"tp": partner}]
    greet += [{"tp": (hi + dh) % highs * 2 + lo} for dh in range(1, highs)]
    greet += [{"grp": (g + dg) % groups} for dg in range(1, groups)]
    greet += [{"ep": (e + de) % eps} for de in range(1, eps)]
    for other in greet:
        pl.semaphore_signal(barrier, inc=1, device_id=other, device_id_type=MESH)
    pl.semaphore_wait(barrier, len(greet))

    def remote(src, dst, sems, index, device):
        return pltpu.make_async_remote_copy(
            src_ref=src,
            dst_ref=dst,
            send_sem=sems.at[(0,) + index],
            recv_sem=sems.at[(1,) + index],
            device_id=device,
            device_id_type=MESH,
        )

    items = []
    half = width // 2
    for source, buffer in ((gate_hbm, gate), (up_hbm, up)):
        for part in range(2):
            items.append((source, buffer, part * half, half, 0, units))
    parts = 4
    slab = width // parts
    for part in range(parts):
        items.append((down_hbm, down, 0, units, part * slab, slab))

    def view(ref, item, piece=None):
        _, _, r0, count, c0, columns = item
        if piece is None:
            return ref.at[pl.ds(r0, count), pl.ds(c0, columns)]
        size = count // groups
        start = pl.multiple_of(r0 + piece * size, 16)
        return ref.at[pl.ds(start, size), pl.ds(c0, columns)]

    def copy_a(i):
        item = items[i]
        return remote(
            view(item[0].at[0], item), view(item[1].at[t], item), sem_a, (i,), {"tp": partner}
        )

    def copy_b(i, dh):
        item = items[i]
        other = (hi + dh) % highs * 2 + lo
        return remote(
            view(item[0].at[0], item, g), view(item[1].at[t], item, g), sem_b, (i, dh), {"tp": other}
        )

    def origin(dh):
        return (hi + highs - dh) % highs * 2 + lo

    def copy_c(i, dh, dg):
        item = items[i]
        ref = view(item[1].at[origin(dh)], item, g)
        return remote(ref, ref, sem_c, (i, dh, dg), {"grp": (g + dg) % groups})

    def copy_d(i, dh):
        item = items[i]
        ref = view(item[1].at[origin(dh)], item, g)
        return remote(ref, ref, sem_d, (i, dh), {"tp": partner})

    def copy_e(i, dh, dg):
        item = items[i]
        ref = view(item[1].at[origin(dh)], item, (g + groups - dg) % groups)
        return remote(ref, ref, sem_e, (i, dh, dg), {"tp": partner})

    count = len(items)
    for i in range(count):
        for dh in range(1, highs):
            copy_b(i, dh).start()
    for i in range(count):
        copy_a(i).start()

    def relay_cross(i):
        for dh in range(1, highs):
            copy_b(i, dh).wait_recv()
            for dg in range(1, groups):
                copy_c(i, dh, dg).start()
            copy_d(i, dh).start()

    def relay_group(i):
        for dh in range(1, highs):
            for dg in range(1, groups):
                copy_c(i, dh, dg).wait_recv()
                copy_e(i, dh, dg).start()

    def arrived(i):
        copy_a(i).wait_recv()
        for dh in range(1, highs):
            copy_d(i, dh).wait_recv()
            for dg in range(1, groups):
                copy_e(i, dh, dg).wait_recv()

    halo_copy = remote(
        conv_hbm.at[pl.ds(rows - halo, halo)],
        ext.at[pl.ds(0, halo)],
        sem_halo,
        (0,),
        {"ep": (e + 1) % eps},
    )

    @pl.when(e < eps - 1)
    def _():
        halo_copy.start()

    @pl.when(e == 0)
    def _():
        ext[0:halo, :] = jnp.zeros((halo, width), BF16)

    ids = jnp.zeros((2, block), jnp.int32)
    weights = jnp.zeros((2, block), F32)
    for q in range(tps):
        span = slice(q * block, (q + 1) * block)
        ids = jnp.where(t == q, ids_ref[:, span], ids)
        weights = jnp.where(t == q, route_ref[:, span], weights)
    experts = max(8, eps)
    kind = lax.broadcasted_iota(jnp.int32, (experts, block), 0)
    above = (
        lax.broadcasted_iota(jnp.int32, (block, block), 0)
        < lax.broadcasted_iota(jnp.int32, (block, block), 1)
    )
    above = jnp.where(above, 1.0, 0.0).astype(BF16)
    slot = lax.broadcasted_iota(jnp.int32, (slots, block), 0).astype(F32)
    seen = jnp.zeros((experts, 1), F32)
    pick = jnp.zeros((slots, block), F32)
    mixing = jnp.zeros((slots, block), F32)
    for k in range(2):
        named = ids[k : k + 1, :]
        onehot = jnp.where(named == kind, 1.0, 0.0)
        before = jnp.dot(onehot.astype(BF16), above, preferred_element_type=F32) + seen
        position = jnp.sum(before * onehot, axis=0, keepdims=True)
        seen = seen + jnp.sum(onehot, axis=1, keepdims=True)
        target = named.astype(F32) * float(cap) + position
        here = jnp.where(target == slot, 1.0, 0.0)
        pick = pick + here
        mixing = mixing + here * weights[k : k + 1, :]
    mix_high = mixing.astype(BF16)
    mix[0] = mix_high
    mix[1] = (mixing - mix_high.astype(F32)).astype(BF16)

    local[0].wait()
    own = own_in[...].astype(F32)
    scale = lax.rsqrt(jnp.mean(own * own, axis=1, keepdims=True) + EPSILON)
    normed = (own * scale * moe_gain[...]).astype(BF16)
    chosen = jnp.dot(pick.astype(BF16), normed, preferred_element_type=F32).astype(BF16)
    send_rows[...] = chosen.reshape(eps, cap, width)

    def copy_x(de):
        other = (e + de) % eps
        return remote(send_rows.at[other], got_rows.at[e], sem_x, (de,), {"ep": other})

    def copy_y(de, part):
        other = (e + de) % eps
        columns = pl.ds(part * slab, slab)
        return remote(
            result.at[other, :, columns],
            back.at[e, :, columns],
            sem_y,
            (de, part),
            {"ep": other},
        )

    for de in range(1, eps):
        copy_x(de).start()
    got_rows[pl.ds(e, 1)] = send_rows[pl.ds(e, 1)]

    local[1].wait()

    def conv_chunk(j):
        row0 = pl.multiple_of(j * CONV_ROWS, CONV_ROWS)
        tall = CONV_ROWS + halo

        def columns_of(c):
            return pl.ds(pl.multiple_of(c * LANES, LANES), LANES)

        def first(c, squares):
            columns = columns_of(c)
            window = ext[pl.ds(row0, tall), columns].astype(F32)
            total = jnp.zeros((CONV_ROWS, LANES), F32)
            for phase in range(8):
                shifts = [k for k in range(halo - reach, halo + 1) if k % 8 == phase]
                top = max(shifts) - phase
                shifted = window[phase : phase + top + CONV_ROWS]
                for k in shifts:
                    tap = taps[pl.ds(k - halo + reach, 1), columns]
                    total = total + shifted[k - phase : k - phase + CONV_ROWS] * tap
            conv_sum[:, columns] = total
            return squares + total * total

        squares = lax.fori_loop(0, width // LANES, first, jnp.zeros((CONV_ROWS, LANES), F32))
        mean = jnp.sum(squares, axis=1, keepdims=True) * (1.0 / width)
        rate = lax.rsqrt(mean + EPSILON)

        def second(c, carry):
            columns = columns_of(c)
            value = conv_sum[:, columns] * rate * conv_gain[:, columns]
            act[pl.ds(row0, CONV_ROWS), columns] = silu(value).astype(BF16)
            return carry

        lax.fori_loop(0, width // LANES, second, 0)

    chunks = rows // CONV_ROWS

    def conv_range(start, stop):
        def step(j, carry):
            conv_chunk(j)
            return carry

        lax.fori_loop(start, stop, step, 0)

    conv_range(1, 2)
    relay_cross(0)
    conv_range(2, 3)
    relay_cross(1)
    conv_range(3, 4)
    relay_group(0)
    conv_range(4, 5)
    relay_cross(2)
    relay_group(1)
    conv_range(5, 6)
    relay_cross(3)
    conv_range(6, EARLY)
    relay_group(2)
    relay_cross(4)
    relay_cross(5)
    for de in range(1, eps):
        copy_x(de).wait_recv()
    local[3].wait()
    arrived(0)
    arrived(1)

    def gates(q, carry):
        gate_val[q] = jnp.dot(
            got_rows[...].reshape(slots, width), gate[q], preferred_element_type=F32
        )
        return carry

    lax.fori_loop(0, tps, gates, 0)
    relay_group(3)
    relay_cross(6)
    relay_cross(7)
    local[4].wait()
    arrived(2)
    arrived(3)

    def ups(q, carry):
        value = jnp.dot(got_rows[...].reshape(slots, width), up[q], preferred_element_type=F32)
        hidden[q] = (silu(gate_val[q]) * value).astype(BF16)
        return carry

    lax.fori_loop(0, tps, ups, 0)
    local[5].wait()
    tile = 256
    for part in range(parts):
        relay_group(4 + part)
        arrived(4 + part)

        def downs(n, carry):
            columns = pl.ds(pl.multiple_of(part * slab + n * tile, tile), tile)
            value = jnp.dot(hidden[0], down[0, :, columns], preferred_element_type=F32)
            for q in range(1, tps):
                value = value + jnp.dot(hidden[q], down[q, :, columns], preferred_element_type=F32)
            result[:, :, columns] = value.astype(BF16).reshape(eps, cap, tile)
            return carry

        lax.fori_loop(0, slab // tile, downs, 0)
        for de in range(1, eps):
            copy_y(de, part).start()
    back[pl.ds(e, 1)] = result[pl.ds(e, 1)]

    conv_range(EARLY, chunks)

    @pl.when(e > 0)
    def _():
        halo_copy.wait_recv()

    conv_range(0, 1)
    local[2].wait()
    out_rows = rows // 2

    def project(j, carry):
        where = pl.ds(pl.multiple_of(j * out_rows, 16), out_rows)
        conv_out[where, :] = jnp.dot(
            act[where, :], convw[...], preferred_element_type=F32
        ).astype(BF16)
        return carry

    lax.fori_loop(0, 2, project, 0)
    for part in range(parts):
        for de in range(1, eps):
            copy_y(de, part).wait_recv()
    every = back[...].reshape(slots, width)
    turned = (((0,), (0,)), ((), ()))
    mixed = lax.dot_general(mix[0], every, turned, preferred_element_type=F32)
    mixed = mixed + lax.dot_general(mix[1], every, turned, preferred_element_type=F32)
    scale = lax.rsqrt(jnp.mean(mixed * mixed, axis=1, keepdims=True) + EPSILON)
    moe_out[...] = (mixed * scale * post_gain[...]).astype(BF16)

    @pl.when(e < eps - 1)
    def _():
        halo_copy.wait_send()

    for i in range(count):
        copy_a(i).wait_send()
        for dh in range(1, highs):
            copy_b(i, dh).wait_send()
            copy_d(i, dh).wait_send()
            for dg in range(1, groups):
                copy_c(i, dh, dg).wait_send()
                copy_e(i, dh, dg).wait_send()
    for de in range(1, eps):
        copy_x(de).wait_send()
        for part in range(parts):
            copy_y(de, part).wait_send()


def body(
    sizes,
    conv_input,
    conv_taps,
    conv_gain,
    conv_weight,
    moe_input,
    moe_gain,
    expert_ids,
    route_weights,
    gate_weight,
    up_weight,
    down_weight,
    post_gain,
):
    groups, eps, tps = sizes
    highs = tps // 2
    rows, width = conv_input.shape
    block = moe_input.shape[0] // tps
    cap = 2 * block // eps
    units = gate_weight.shape[2]
    halo = (conv_taps.shape[0] - 1 + 15) // 16 * 16
    vmem = pl.BlockSpec(memory_space=pltpu.VMEM)
    hbm = pl.BlockSpec(memory_space=pl.ANY)
    dma = pltpu.SemaphoreType.DMA
    items = 8
    call = pl.pallas_call(
        functools.partial(kernel, sizes),
        out_shape=(
            jax.ShapeDtypeStruct((rows, conv_weight.shape[1]), BF16),
            jax.ShapeDtypeStruct((block, width), BF16),
        ),
        in_specs=[hbm, vmem, vmem, hbm, hbm, vmem, vmem, vmem, hbm, hbm, hbm, vmem],
        out_specs=(vmem, vmem),
        scratch_shapes=[
            pltpu.VMEM((rows + halo, width), BF16),
            pltpu.VMEM(conv_weight.shape, BF16),
            pltpu.VMEM((rows, width), BF16),
            pltpu.VMEM((CONV_ROWS, width), F32),
            pltpu.VMEM((block, width), BF16),
            pltpu.VMEM((tps, width, units), BF16),
            pltpu.VMEM((tps, width, units), BF16),
            pltpu.VMEM((tps, units, width), BF16),
            pltpu.VMEM((2, 2 * block, block), BF16),
            pltpu.VMEM((eps, cap, width), BF16),
            pltpu.VMEM((eps, cap, width), BF16),
            pltpu.VMEM((tps, 2 * block, units), F32),
            pltpu.VMEM((tps, 2 * block, units), BF16),
            pltpu.VMEM((eps, cap, width), BF16),
            pltpu.VMEM((eps, cap, width), BF16),
            dma((6,)),
            dma((2, 1)),
            dma((2, items)),
            dma((2, items, highs)),
            dma((2, items, highs, groups)),
            dma((2, items, highs)),
            dma((2, items, highs, groups)),
            dma((2, eps)),
            dma((2, eps, 4)),
        ],
        compiler_params=pltpu.CompilerParams(
            collective_id=0, has_side_effects=True, vmem_limit_bytes=60 * 1024 * 1024
        ),
    )
    return call(
        conv_input,
        conv_taps,
        conv_gain.reshape(1, width),
        conv_weight,
        moe_input,
        moe_gain.reshape(1, width),
        expert_ids.T,
        route_weights.T,
        gate_weight,
        up_weight,
        down_weight,
        post_gain.reshape(1, width),
    )


def solution(mesh):
    in_specs = (
        P(("grp", "ep"), None),
        P(),
        P(),
        P(None, "tp"),
        P(("grp", "ep"), None),
        P(),
        P(("grp", "ep"), None),
        P(("grp", "ep"), None),
        P("ep", None, "tp"),
        P("ep", None, "tp"),
        P("ep", "tp", None),
        P(),
    )
    out_specs = (P(("grp", "ep"), "tp"), P(("grp", "ep", "tp"), None))
    sizes = (mesh.shape["grp"], mesh.shape["ep"], mesh.shape["tp"])
    return jax.shard_map(
        functools.partial(body, sizes),
        mesh=mesh,
        in_specs=in_specs,
        out_specs=out_specs,
        check_vma=False,
    )
```

```python
import functools

import jax
import jax.numpy as jnp
from jax import lax
from jax.experimental import pallas as pl
from jax.experimental.pallas import tpu as pltpu
from jax.sharding import PartitionSpec as P

EPSILON = 1e-06
MESH = pl.DeviceIdType.MESH
F32, BF16 = jnp.float32, jnp.bfloat16
CONV_ROWS = 64
LANES = 128
PARTS = 4
PAIR = 2


def silu(v):
    return v / (1.0 + jnp.exp(-v))


def kernel(
    sizes,
    conv_hbm,
    taps,
    conv_gain,
    convw_hbm,
    moe_hbm,
    moe_gain,
    ids_ref,
    route_ref,
    gate_hbm,
    up_hbm,
    down_hbm,
    post_gain,
    conv_out,
    moe_out,
    ext,
    convw,
    act,
    conv_sum,
    window,
    own_in,
    gate,
    up,
    down,
    mix,
    send_rows,
    got_rows,
    gate_val,
    hidden,
    result,
    back,
    sem_local,
    sem_halo,
    sem_a,
    sem_b,
    sem_c,
    sem_d,
    sem_e,
    sem_x,
    sem_y,
):
    groups, eps, tps = sizes
    highs = tps // 2
    g, e, t = lax.axis_index("grp"), lax.axis_index("ep"), lax.axis_index("tp")
    hi, lo = t // 2, t % 2
    partner = hi * 2 + (1 - lo)
    rows = conv_hbm.shape[0]
    width = conv_hbm.shape[1]
    reach = taps.shape[0] - 1
    halo = ext.shape[0] - rows
    block = own_in.shape[0]
    slots = 2 * block
    cap = slots // eps
    units = gate.shape[2]

    local = [
        pltpu.make_async_copy(
            moe_hbm.at[pl.ds(pl.multiple_of(t * block, 16), block)], own_in, sem_local.at[0]
        ),
        pltpu.make_async_copy(conv_hbm, ext.at[pl.ds(halo, rows)], sem_local.at[1]),
        pltpu.make_async_copy(convw_hbm, convw, sem_local.at[2]),
        pltpu.make_async_copy(gate_hbm.at[0], gate.at[t], sem_local.at[3]),
        pltpu.make_async_copy(up_hbm.at[0], up.at[t], sem_local.at[4]),
        pltpu.make_async_copy(down_hbm.at[0], down.at[t], sem_local.at[5]),
    ]
    for copy in local:
        copy.start()

    barrier = pltpu.get_barrier_semaphore()
    greet = [{"tp": partner}]
    greet += [{"tp": (hi + dh) % highs * 2 + lo} for dh in range(1, highs)]
    greet += [{"grp": (g + dg) % groups} for dg in range(1, groups)]
    greet += [{"ep": (e + de) % eps} for de in range(1, eps)]
    for other in greet:
        pl.semaphore_signal(barrier, inc=1, device_id=other, device_id_type=MESH)
    pl.semaphore_wait(barrier, len(greet))

    def remote(src, dst, sems, index, device):
        return pltpu.make_async_remote_copy(
            src_ref=src,
            dst_ref=dst,
            send_sem=sems.at[(0,) + index],
            recv_sem=sems.at[(1,) + index],
            device_id=device,
            device_id_type=MESH,
        )

    items = []
    parts = PARTS
    slab = width // parts
    for source, buffer in ((gate_hbm, gate), (up_hbm, up)):
        for part in range(parts):
            items.append((source, buffer, part * slab, slab, 0, units))
    for part in range(parts):
        items.append((down_hbm, down, 0, units, part * slab, slab))

    def view(ref, item, piece=None):
        _, _, r0, count, c0, columns = item
        if piece is None:
            return ref.at[pl.ds(r0, count), pl.ds(c0, columns)]
        size = count // groups
        start = pl.multiple_of(r0 + piece * size, 16)
        return ref.at[pl.ds(start, size), pl.ds(c0, columns)]

    def copy_a(i):
        item = items[i]
        return remote(
            view(item[0].at[0], item), view(item[1].at[t], item), sem_a, (i,), {"tp": partner}
        )

    def copy_b(i, dh):
        item = items[i]
        other = (hi + dh) % highs * 2 + lo
        return remote(
            view(item[0].at[0], item, g), view(item[1].at[t], item, g), sem_b, (i, dh), {"tp": other}
        )

    def origin(dh):
        return (hi + highs - dh) % highs * 2 + lo

    def copy_c(i, dh, dg):
        item = items[i]
        ref = view(item[1].at[origin(dh)], item, g)
        return remote(ref, ref, sem_c, (i, dh, dg), {"grp": (g + dg) % groups})

    def copy_d(i, dh):
        item = items[i]
        ref = view(item[1].at[origin(dh)], item, g)
        return remote(ref, ref, sem_d, (i, dh), {"tp": partner})

    def copy_e(i, dh, dg):
        item = items[i]
        ref = view(item[1].at[origin(dh)], item, (g + groups - dg) % groups)
        return remote(ref, ref, sem_e, (i, dh, dg), {"tp": partner})

    count = len(items)
    for i in range(count):
        for dh in range(1, highs):
            copy_b(i, dh).start()
    for i in range(count):
        copy_a(i).start()

    def relay_cross(i):
        for dh in range(1, highs):
            copy_b(i, dh).wait_recv()
            for dg in range(1, groups):
                copy_c(i, dh, dg).start()
            copy_d(i, dh).start()

    def relay_group(i):
        for dh in range(1, highs):
            for dg in range(1, groups):
                copy_c(i, dh, dg).wait_recv()
                copy_e(i, dh, dg).start()

    def arrived(i):
        copy_a(i).wait_recv()
        for dh in range(1, highs):
            copy_d(i, dh).wait_recv()
            for dg in range(1, groups):
                copy_e(i, dh, dg).wait_recv()

    halo_copy = remote(
        conv_hbm.at[pl.ds(rows - halo, halo)],
        ext.at[pl.ds(0, halo)],
        sem_halo,
        (0,),
        {"ep": (e + 1) % eps},
    )

    @pl.when(e < eps - 1)
    def _():
        halo_copy.start()

    @pl.when(e == 0)
    def _():
        ext[0:halo, :] = jnp.zeros((halo, width), BF16)

    ids = jnp.zeros((2, block), jnp.int32)
    weights = jnp.zeros((2, block), F32)
    for q in range(tps):
        span = slice(q * block, (q + 1) * block)
        ids = jnp.where(t == q, ids_ref[:, span], ids)
        weights = jnp.where(t == q, route_ref[:, span], weights)
    experts = max(8, eps)
    kind = lax.broadcasted_iota(jnp.int32, (experts, block), 0)
    above = (
        lax.broadcasted_iota(jnp.int32, (block, block), 0)
        < lax.broadcasted_iota(jnp.int32, (block, block), 1)
    )
    above = jnp.where(above, 1.0, 0.0).astype(BF16)
    slot = lax.broadcasted_iota(jnp.int32, (slots, block), 0).astype(F32)
    seen = jnp.zeros((experts, 1), F32)
    pick = jnp.zeros((slots, block), F32)
    mixing = jnp.zeros((slots, block), F32)
    for k in range(2):
        named = ids[k : k + 1, :]
        onehot = jnp.where(named == kind, 1.0, 0.0)
        before = jnp.dot(onehot.astype(BF16), above, preferred_element_type=F32) + seen
        position = jnp.sum(before * onehot, axis=0, keepdims=True)
        seen = seen + jnp.sum(onehot, axis=1, keepdims=True)
        target = named.astype(F32) * float(cap) + position
        here = jnp.where(target == slot, 1.0, 0.0)
        pick = pick + here
        mixing = mixing + here * weights[k : k + 1, :]
    mix_high = mixing.astype(BF16)
    mix[0] = mix_high
    mix[1] = (mixing - mix_high.astype(F32)).astype(BF16)

    local[0].wait()
    own = own_in[...].astype(F32)
    scale = lax.rsqrt(jnp.mean(own * own, axis=1, keepdims=True) + EPSILON)
    normed = (own * scale * moe_gain[...]).astype(BF16)
    chosen = jnp.dot(pick.astype(BF16), normed, preferred_element_type=F32).astype(BF16)
    send_rows[...] = chosen.reshape(eps, cap, width)

    def copy_x(de):
        other = (e + de) % eps
        return remote(send_rows.at[other], got_rows.at[e], sem_x, (de,), {"ep": other})

    def copy_y(de, part):
        other = (e + de) % eps
        columns = pl.ds(part * slab, slab)
        return remote(
            result.at[other, :, columns],
            back.at[e, :, columns],
            sem_y,
            (de, part),
            {"ep": other},
        )

    for de in range(1, eps):
        copy_x(de).start()
    got_rows[pl.ds(e, 1)] = send_rows[pl.ds(e, 1)]

    local[1].wait()

    def conv_chunk(j):
        row0 = pl.multiple_of(j * CONV_ROWS, CONV_ROWS)
        tall = CONV_ROWS + halo

        def columns_of(c):
            return pl.ds(pl.multiple_of(c * LANES, LANES), LANES)

        def first(pair, squares):
            for side in range(PAIR):
                columns = columns_of(pair * PAIR + side)
                window[side] = ext[pl.ds(row0, tall), columns].astype(F32)
            for side in range(PAIR):
                columns = columns_of(pair * PAIR + side)
                total = jnp.zeros((CONV_ROWS, LANES), F32)
                for k in range(reach + 1):
                    shifted = window[side, pl.ds(halo - reach + k, CONV_ROWS), :]
                    total = total + shifted * taps[pl.ds(k, 1), columns]
                conv_sum[:, columns] = total
                squares = squares + total * total
            return squares

        start = jnp.zeros((CONV_ROWS, LANES), F32)
        squares = lax.fori_loop(0, width // LANES // PAIR, first, start)
        mean = jnp.sum(squares, axis=1, keepdims=True) * (1.0 / width)
        rate = lax.rsqrt(mean + EPSILON)

        def second(c, carry):
            columns = columns_of(c)
            value = conv_sum[:, columns] * rate * conv_gain[:, columns]
            act[pl.ds(row0, CONV_ROWS), columns] = silu(value).astype(BF16)
            return carry

        lax.fori_loop(0, width // LANES, second, 0)

    chunks = rows // CONV_ROWS

    def conv_range(start, stop):
        def step(j, carry):
            conv_chunk(j)
            return carry

        lax.fori_loop(start, stop, step, 0)

    def step(i):
        relay_cross(i)
        if i > 0:
            relay_group(i - 1)

    early = min(chunks, 2 * parts + 1)
    for i in range(2 * parts):
        if 1 + i < early:
            conv_range(1 + i, 2 + i)
        step(i)
    step(2 * parts)
    for de in range(1, eps):
        copy_x(de).wait_recv()
    local[3].wait()
    for i in range(parts):
        arrived(i)

    def gates(q, carry):
        gate_val[q] = jnp.dot(
            got_rows[...].reshape(slots, width), gate[q], preferred_element_type=F32
        )
        return carry

    lax.fori_loop(0, tps, gates, 0)
    step(2 * parts + 1)
    local[4].wait()
    for i in range(parts):
        arrived(parts + i)

    def ups(q, carry):
        value = jnp.dot(got_rows[...].reshape(slots, width), up[q], preferred_element_type=F32)
        hidden[q] = (silu(gate_val[q]) * value).astype(BF16)
        return carry

    lax.fori_loop(0, tps, ups, 0)
    local[5].wait()
    tile = 256
    for part in range(parts):
        if part + 1 == parts:
            relay_group(count - 1)
        arrived(2 * parts + part)

        def downs(n, carry):
            columns = pl.ds(pl.multiple_of(part * slab + n * tile, tile), tile)
            value = jnp.dot(hidden[0], down[0, :, columns], preferred_element_type=F32)
            for q in range(1, tps):
                value = value + jnp.dot(hidden[q], down[q, :, columns], preferred_element_type=F32)
            result[:, :, columns] = value.astype(BF16).reshape(eps, cap, tile)
            return carry

        lax.fori_loop(0, slab // tile, downs, 0)
        for de in range(1, eps):
            copy_y(de, part).start()
        if part + 2 < parts:
            step(2 * parts + 2 + part)
    back[pl.ds(e, 1)] = result[pl.ds(e, 1)]

    if early < chunks:
        conv_range(early, chunks)

    @pl.when(e > 0)
    def _():
        halo_copy.wait_recv()

    conv_range(0, 1)
    local[2].wait()
    out_rows = rows // 2

    def project(j, carry):
        where = pl.ds(pl.multiple_of(j * out_rows, 16), out_rows)
        conv_out[where, :] = jnp.dot(
            act[where, :], convw[...], preferred_element_type=F32
        ).astype(BF16)
        return carry

    lax.fori_loop(0, 2, project, 0)
    for part in range(parts):
        for de in range(1, eps):
            copy_y(de, part).wait_recv()
    every = back[...].reshape(slots, width)
    turned = (((0,), (0,)), ((), ()))
    mixed = lax.dot_general(mix[0], every, turned, preferred_element_type=F32)
    mixed = mixed + lax.dot_general(mix[1], every, turned, preferred_element_type=F32)
    scale = lax.rsqrt(jnp.mean(mixed * mixed, axis=1, keepdims=True) + EPSILON)
    moe_out[...] = (mixed * scale * post_gain[...]).astype(BF16)

    @pl.when(e < eps - 1)
    def _():
        halo_copy.wait_send()

    for i in range(count):
        copy_a(i).wait_send()
        for dh in range(1, highs):
            copy_b(i, dh).wait_send()
            copy_d(i, dh).wait_send()
            for dg in range(1, groups):
                copy_c(i, dh, dg).wait_send()
                copy_e(i, dh, dg).wait_send()
    for de in range(1, eps):
        copy_x(de).wait_send()
        for part in range(parts):
            copy_y(de, part).wait_send()


def body(
    sizes,
    conv_input,
    conv_taps,
    conv_gain,
    conv_weight,
    moe_input,
    moe_gain,
    expert_ids,
    route_weights,
    gate_weight,
    up_weight,
    down_weight,
    post_gain,
):
    groups, eps, tps = sizes
    highs = tps // 2
    rows, width = conv_input.shape
    block = moe_input.shape[0] // tps
    cap = 2 * block // eps
    units = gate_weight.shape[2]
    halo = (conv_taps.shape[0] - 1 + 15) // 16 * 16
    vmem = pl.BlockSpec(memory_space=pltpu.VMEM)
    hbm = pl.BlockSpec(memory_space=pl.ANY)
    dma = pltpu.SemaphoreType.DMA
    items = 3 * PARTS
    call = pl.pallas_call(
        functools.partial(kernel, sizes),
        out_shape=(
            jax.ShapeDtypeStruct((rows, conv_weight.shape[1]), BF16),
            jax.ShapeDtypeStruct((block, width), BF16),
        ),
        in_specs=[hbm, vmem, vmem, hbm, hbm, vmem, vmem, vmem, hbm, hbm, hbm, vmem],
        out_specs=(vmem, vmem),
        scratch_shapes=[
            pltpu.VMEM((rows + halo, width), BF16),
            pltpu.VMEM(conv_weight.shape, BF16),
            pltpu.VMEM((rows, width), BF16),
            pltpu.VMEM((CONV_ROWS, width), F32),
            pltpu.VMEM((PAIR, CONV_ROWS + halo, LANES), F32),
            pltpu.VMEM((block, width), BF16),
            pltpu.VMEM((tps, width, units), BF16),
            pltpu.VMEM((tps, width, units), BF16),
            pltpu.VMEM((tps, units, width), BF16),
            pltpu.VMEM((2, 2 * block, block), BF16),
            pltpu.VMEM((eps, cap, width), BF16),
            pltpu.VMEM((eps, cap, width), BF16),
            pltpu.VMEM((tps, 2 * block, units), F32),
            pltpu.VMEM((tps, 2 * block, units), BF16),
            pltpu.VMEM((eps, cap, width), BF16),
            pltpu.VMEM((eps, cap, width), BF16),
            dma((6,)),
            dma((2, 1)),
            dma((2, items)),
            dma((2, items, highs)),
            dma((2, items, highs, groups)),
            dma((2, items, highs)),
            dma((2, items, highs, groups)),
            dma((2, eps)),
            dma((2, eps, PARTS)),
        ],
        compiler_params=pltpu.CompilerParams(
            collective_id=0, has_side_effects=True, vmem_limit_bytes=60 * 1024 * 1024
        ),
    )
    return call(
        conv_input,
        conv_taps,
        conv_gain.reshape(1, width),
        conv_weight,
        moe_input,
        moe_gain.reshape(1, width),
        expert_ids.T,
        route_weights.T,
        gate_weight,
        up_weight,
        down_weight,
        post_gain.reshape(1, width),
    )


def solution(mesh):
    in_specs = (
        P(("grp", "ep"), None),
        P(),
        P(),
        P(None, "tp"),
        P(("grp", "ep"), None),
        P(),
        P(("grp", "ep"), None),
        P(("grp", "ep"), None),
        P("ep", None, "tp"),
        P("ep", None, "tp"),
        P("ep", "tp", None),
        P(),
    )
    out_specs = (P(("grp", "ep"), "tp"), P(("grp", "ep", "tp"), None))
    sizes = (mesh.shape["grp"], mesh.shape["ep"], mesh.shape["tp"])
    return jax.shard_map(
        functools.partial(body, sizes),
        mesh=mesh,
        in_specs=in_specs,
        out_specs=out_specs,
        check_vma=False,
    )
```

```python
import functools

import jax
import jax.numpy as jnp
from jax import lax
from jax.experimental import pallas as pl
from jax.experimental.pallas import tpu as pltpu
from jax.sharding import PartitionSpec as P

EPSILON = 1e-06
MESH = pl.DeviceIdType.MESH
F32, BF16 = jnp.float32, jnp.bfloat16
CONV_ROWS = 64
LANES = 128
PARTS = 4
PAIR = 2


def silu(v):
    return v / (1.0 + jnp.exp(-v))


def kernel(
    sizes,
    conv_hbm,
    taps,
    conv_gain,
    convw_hbm,
    moe_hbm,
    moe_gain,
    ids_ref,
    route_ref,
    gate_hbm,
    up_hbm,
    down_hbm,
    post_gain,
    conv_out,
    moe_out,
    ext,
    convw,
    act,
    conv_sum,
    window,
    own_in,
    gate,
    up,
    down,
    mix,
    send_rows,
    got_rows,
    gate_val,
    hidden,
    result,
    back,
    sem_local,
    sem_halo,
    sem_a,
    sem_b,
    sem_c,
    sem_d,
    sem_e,
    sem_x,
    sem_y,
):
    groups, eps, tps = sizes
    highs = tps // 2
    g, e, t = lax.axis_index("grp"), lax.axis_index("ep"), lax.axis_index("tp")
    hi, lo = t // 2, t % 2
    partner = hi * 2 + (1 - lo)
    rows = conv_hbm.shape[0]
    width = conv_hbm.shape[1]
    reach = taps.shape[0] - 1
    halo = ext.shape[0] - rows
    block = own_in.shape[0]
    slots = 2 * block
    cap = slots // eps
    units = gate.shape[2]

    local = [
        pltpu.make_async_copy(
            moe_hbm.at[pl.ds(pl.multiple_of(t * block, 16), block)], own_in, sem_local.at[0]
        ),
        pltpu.make_async_copy(conv_hbm, ext.at[pl.ds(halo, rows)], sem_local.at[1]),
        pltpu.make_async_copy(convw_hbm, convw, sem_local.at[2]),
        pltpu.make_async_copy(gate_hbm.at[0], gate.at[t], sem_local.at[3]),
        pltpu.make_async_copy(up_hbm.at[0], up.at[t], sem_local.at[4]),
        pltpu.make_async_copy(down_hbm.at[0], down.at[t], sem_local.at[5]),
    ]
    for copy in local:
        copy.start()

    barrier = pltpu.get_barrier_semaphore()
    greet = [{"tp": partner}]
    greet += [{"tp": (hi + dh) % highs * 2 + lo} for dh in range(1, highs)]
    greet += [{"grp": (g + dg) % groups} for dg in range(1, groups)]
    greet += [{"ep": (e + de) % eps} for de in range(1, eps)]
    for other in greet:
        pl.semaphore_signal(barrier, inc=1, device_id=other, device_id_type=MESH)
    pl.semaphore_wait(barrier, len(greet))

    def remote(src, dst, sems, index, device):
        return pltpu.make_async_remote_copy(
            src_ref=src,
            dst_ref=dst,
            send_sem=sems.at[(0,) + index],
            recv_sem=sems.at[(1,) + index],
            device_id=device,
            device_id_type=MESH,
        )

    items = []
    parts = PARTS
    slab = width // parts
    for source, buffer in ((gate_hbm, gate), (up_hbm, up)):
        for part in range(parts):
            items.append((source, buffer, part * slab, slab, 0, units))
    for part in range(parts):
        items.append((down_hbm, down, 0, units, part * slab, slab))

    def view(ref, item, piece=None):
        _, _, r0, count, c0, columns = item
        if piece is None:
            return ref.at[pl.ds(r0, count), pl.ds(c0, columns)]
        size = count // groups
        start = pl.multiple_of(r0 + piece * size, 16)
        return ref.at[pl.ds(start, size), pl.ds(c0, columns)]

    def copy_a(i):
        item = items[i]
        return remote(
            view(item[0].at[0], item), view(item[1].at[t], item), sem_a, (i,), {"tp": partner}
        )

    def copy_b(i, dh):
        item = items[i]
        other = (hi + dh) % highs * 2 + lo
        return remote(
            view(item[0].at[0], item, g), view(item[1].at[t], item, g), sem_b, (i, dh), {"tp": other}
        )

    def origin(dh):
        return (hi + highs - dh) % highs * 2 + lo

    def copy_c(i, dh, dg):
        item = items[i]
        ref = view(item[1].at[origin(dh)], item, g)
        return remote(ref, ref, sem_c, (i, dh, dg), {"grp": (g + dg) % groups})

    def copy_d(i, dh):
        item = items[i]
        ref = view(item[1].at[origin(dh)], item, g)
        return remote(ref, ref, sem_d, (i, dh), {"tp": partner})

    def copy_e(i, dh, dg):
        item = items[i]
        ref = view(item[1].at[origin(dh)], item, (g + groups - dg) % groups)
        return remote(ref, ref, sem_e, (i, dh, dg), {"tp": partner})

    count = len(items)
    for i in range(count):
        for dh in range(1, highs):
            copy_b(i, dh).start()
    for i in range(count):
        copy_a(i).start()

    def relay_cross(i):
        for dh in range(1, highs):
            copy_b(i, dh).wait_recv()
            for dg in range(1, groups):
                copy_c(i, dh, dg).start()
            copy_d(i, dh).start()

    def relay_group(i):
        for dh in range(1, highs):
            for dg in range(1, groups):
                copy_c(i, dh, dg).wait_recv()
                copy_e(i, dh, dg).start()

    def arrived(i):
        copy_a(i).wait_recv()
        for dh in range(1, highs):
            copy_d(i, dh).wait_recv()
            for dg in range(1, groups):
                copy_e(i, dh, dg).wait_recv()

    halo_copy = remote(
        conv_hbm.at[pl.ds(rows - halo, halo)],
        ext.at[pl.ds(0, halo)],
        sem_halo,
        (0,),
        {"ep": (e + 1) % eps},
    )

    @pl.when(e < eps - 1)
    def _():
        halo_copy.start()

    @pl.when(e == 0)
    def _():
        ext[0:halo, :] = jnp.zeros((halo, width), BF16)

    ids = jnp.zeros((2, block), jnp.int32)
    weights = jnp.zeros((2, block), F32)
    for q in range(tps):
        span = slice(q * block, (q + 1) * block)
        ids = jnp.where(t == q, ids_ref[:, span], ids)
        weights = jnp.where(t == q, route_ref[:, span], weights)
    experts = max(8, eps)
    kind = lax.broadcasted_iota(jnp.int32, (experts, block), 0)
    above = (
        lax.broadcasted_iota(jnp.int32, (block, block), 0)
        < lax.broadcasted_iota(jnp.int32, (block, block), 1)
    )
    above = jnp.where(above, 1.0, 0.0).astype(BF16)
    slot = lax.broadcasted_iota(jnp.int32, (slots, block), 0).astype(F32)
    seen = jnp.zeros((experts, 1), F32)
    pick = jnp.zeros((slots, block), F32)
    mixing = jnp.zeros((slots, block), F32)
    for k in range(2):
        named = ids[k : k + 1, :]
        onehot = jnp.where(named == kind, 1.0, 0.0)
        before = jnp.dot(onehot.astype(BF16), above, preferred_element_type=F32) + seen
        position = jnp.sum(before * onehot, axis=0, keepdims=True)
        seen = seen + jnp.sum(onehot, axis=1, keepdims=True)
        target = named.astype(F32) * float(cap) + position
        here = jnp.where(target == slot, 1.0, 0.0)
        pick = pick + here
        mixing = mixing + here * weights[k : k + 1, :]
    mix_high = mixing.astype(BF16)
    mix[0] = mix_high
    mix[1] = (mixing - mix_high.astype(F32)).astype(BF16)

    local[0].wait()
    own = own_in[...].astype(F32)
    scale = lax.rsqrt(jnp.mean(own * own, axis=1, keepdims=True) + EPSILON)
    normed = (own * scale * moe_gain[...]).astype(BF16)
    chosen = jnp.dot(pick.astype(BF16), normed, preferred_element_type=F32).astype(BF16)
    send_rows[...] = chosen.reshape(eps, cap, width)

    def copy_x(de):
        other = (e + de) % eps
        return remote(send_rows.at[other], got_rows.at[e], sem_x, (de,), {"ep": other})

    def copy_y(de, part):
        other = (e + de) % eps
        columns = pl.ds(part * slab, slab)
        return remote(
            result.at[other, :, columns],
            back.at[e, :, columns],
            sem_y,
            (de, part),
            {"ep": other},
        )

    for de in range(1, eps):
        copy_x(de).start()
    got_rows[pl.ds(e, 1)] = send_rows[pl.ds(e, 1)]

    local[1].wait()

    def conv_chunk(j):
        row0 = pl.multiple_of(j * CONV_ROWS, CONV_ROWS)
        tall = CONV_ROWS + halo

        def columns_of(c):
            return pl.ds(pl.multiple_of(c * LANES, LANES), LANES)

        def first(pair, squares):
            for side in range(PAIR):
                columns = columns_of(pair * PAIR + side)
                window[side] = ext[pl.ds(row0, tall), columns].astype(F32)
            for side in range(PAIR):
                columns = columns_of(pair * PAIR + side)
                total = jnp.zeros((CONV_ROWS, LANES), F32)
                for k in range(reach + 1):
                    shifted = window[side, pl.ds(halo - reach + k, CONV_ROWS), :]
                    total = total + shifted * taps[pl.ds(k, 1), columns]
                conv_sum[:, columns] = total
                squares = squares + total * total
            return squares

        start = jnp.zeros((CONV_ROWS, LANES), F32)
        squares = lax.fori_loop(0, width // LANES // PAIR, first, start)
        mean = jnp.sum(squares, axis=1, keepdims=True) * (1.0 / width)
        rate = lax.rsqrt(mean + EPSILON)

        def second(c, carry):
            columns = columns_of(c)
            value = conv_sum[:, columns] * rate * conv_gain[:, columns]
            act[pl.ds(row0, CONV_ROWS), columns] = silu(value).astype(BF16)
            return carry

        lax.fori_loop(0, width // LANES, second, 0)

    chunks = rows // CONV_ROWS

    def conv_range(start, stop):
        def step(j, carry):
            conv_chunk(j)
            return carry

        lax.fori_loop(start, stop, step, 0)

    def step(i):
        relay_cross(i)
        if i > 0:
            relay_group(i - 1)

    early = min(chunks, 2 * parts + 1)
    for i in range(2 * parts):
        if 1 + i < early:
            conv_range(1 + i, 2 + i)
        step(i)
    step(2 * parts)
    for de in range(1, eps):
        copy_x(de).wait_recv()
    local[3].wait()
    for i in range(parts):
        arrived(i)

    def gates(q, carry):
        gate_val[q] = jnp.dot(
            got_rows[...].reshape(slots, width), gate[q], preferred_element_type=F32
        )
        return carry

    lax.fori_loop(0, tps, gates, 0)
    step(2 * parts + 1)
    local[4].wait()
    for i in range(parts):
        arrived(parts + i)

    def ups(q, carry):
        value = jnp.dot(got_rows[...].reshape(slots, width), up[q], preferred_element_type=F32)
        hidden[q] = (silu(gate_val[q]) * value).astype(BF16)
        return carry

    lax.fori_loop(0, tps, ups, 0)
    local[5].wait()
    tile = 256
    for part in range(parts):
        if part + 1 == parts:
            relay_group(count - 1)
        arrived(2 * parts + part)

        def downs(n, carry):
            columns = pl.ds(pl.multiple_of(part * slab + n * tile, tile), tile)
            value = jnp.dot(hidden[0], down[0, :, columns], preferred_element_type=F32)
            for q in range(1, tps):
                value = value + jnp.dot(hidden[q], down[q, :, columns], preferred_element_type=F32)
            result[:, :, columns] = value.astype(BF16).reshape(eps, cap, tile)
            return carry

        lax.fori_loop(0, slab // tile, downs, 0)
        for de in range(1, eps):
            copy_y(de, part).start()
        if part + 2 < parts:
            step(2 * parts + 2 + part)
    back[pl.ds(e, 1)] = result[pl.ds(e, 1)]

    if early < chunks:
        conv_range(early, chunks)

    @pl.when(e > 0)
    def _():
        halo_copy.wait_recv()

    conv_range(0, 1)
    local[2].wait()
    out_rows = rows // 2

    def project(j, carry):
        where = pl.ds(pl.multiple_of(j * out_rows, 16), out_rows)
        conv_out[where, :] = jnp.dot(
            act[where, :], convw[...], preferred_element_type=F32
        ).astype(BF16)
        return carry

    lax.fori_loop(0, 2, project, 0)
    for part in range(parts):
        for de in range(1, eps):
            copy_y(de, part).wait_recv()
    every = back[...].reshape(slots, width)
    turned = (((0,), (0,)), ((), ()))
    mixed = lax.dot_general(mix[0], every, turned, preferred_element_type=F32)
    mixed = mixed + lax.dot_general(mix[1], every, turned, preferred_element_type=F32)
    scale = lax.rsqrt(jnp.mean(mixed * mixed, axis=1, keepdims=True) + EPSILON)
    moe_out[...] = (mixed * scale * post_gain[...]).astype(BF16)

    @pl.when(e < eps - 1)
    def _():
        halo_copy.wait_send()

    for i in range(count):
        copy_a(i).wait_send()
        for dh in range(1, highs):
            copy_b(i, dh).wait_send()
            copy_d(i, dh).wait_send()
            for dg in range(1, groups):
                copy_c(i, dh, dg).wait_send()
                copy_e(i, dh, dg).wait_send()
    for de in range(1, eps):
        copy_x(de).wait_send()
        for part in range(parts):
            copy_y(de, part).wait_send()


def body(
    sizes,
    conv_input,
    conv_taps,
    conv_gain,
    conv_weight,
    moe_input,
    moe_gain,
    expert_ids,
    route_weights,
    gate_weight,
    up_weight,
    down_weight,
    post_gain,
):
    groups, eps, tps = sizes
    highs = tps // 2
    rows, width = conv_input.shape
    block = moe_input.shape[0] // tps
    cap = 2 * block // eps
    units = gate_weight.shape[2]
    halo = (conv_taps.shape[0] - 1 + 15) // 16 * 16
    vmem = pl.BlockSpec(memory_space=pltpu.VMEM)
    hbm = pl.BlockSpec(memory_space=pl.ANY)
    dma = pltpu.SemaphoreType.DMA
    items = 3 * PARTS
    call = pl.pallas_call(
        functools.partial(kernel, sizes),
        out_shape=(
            jax.ShapeDtypeStruct((rows, conv_weight.shape[1]), BF16),
            jax.ShapeDtypeStruct((block, width), BF16),
        ),
        in_specs=[hbm, vmem, vmem, hbm, hbm, vmem, vmem, vmem, hbm, hbm, hbm, vmem],
        out_specs=(vmem, vmem),
        scratch_shapes=[
            pltpu.VMEM((rows + halo, width), BF16),
            pltpu.VMEM(conv_weight.shape, BF16),
            pltpu.VMEM((rows, width), BF16),
            pltpu.VMEM((CONV_ROWS, width), F32),
            pltpu.VMEM((PAIR, CONV_ROWS + halo, LANES), F32),
            pltpu.VMEM((block, width), BF16),
            pltpu.VMEM((tps, width, units), BF16),
            pltpu.VMEM((tps, width, units), BF16),
            pltpu.VMEM((tps, units, width), BF16),
            pltpu.VMEM((2, 2 * block, block), BF16),
            pltpu.VMEM((eps, cap, width), BF16),
            pltpu.VMEM((eps, cap, width), BF16),
            pltpu.VMEM((tps, 2 * block, units), F32),
            pltpu.VMEM((tps, 2 * block, units), BF16),
            pltpu.VMEM((eps, cap, width), BF16),
            pltpu.VMEM((eps, cap, width), BF16),
            dma((6,)),
            dma((2, 1)),
            dma((2, items)),
            dma((2, items, highs)),
            dma((2, items, highs, groups)),
            dma((2, items, highs)),
            dma((2, items, highs, groups)),
            dma((2, eps)),
            dma((2, eps, PARTS)),
        ],
        compiler_params=pltpu.CompilerParams(
            collective_id=0, has_side_effects=True, vmem_limit_bytes=60 * 1024 * 1024
        ),
    )
    conv_part, moe_part = call(
        conv_input,
        conv_taps,
        conv_gain.reshape(1, width),
        conv_weight,
        moe_input,
        moe_gain.reshape(1, width),
        expert_ids.T,
        route_weights.T,
        gate_weight,
        up_weight,
        down_weight,
        post_gain.reshape(1, width),
    )
    return pl.pallas_call(
        finish,
        out_shape=(
            jax.ShapeDtypeStruct(conv_part.shape, BF16),
            jax.ShapeDtypeStruct(moe_part.shape, BF16),
        ),
        in_specs=[vmem, vmem],
        out_specs=(vmem, vmem),
        compiler_params=pltpu.CompilerParams(vmem_limit_bytes=16 * 1024 * 1024),
    )(conv_part, moe_part)


def finish(conv_part, moe_part, conv_out, moe_out):
    conv_out[...] = conv_part[...]
    moe_out[...] = moe_part[...]


def solution(mesh):
    in_specs = (
        P(("grp", "ep"), None),
        P(),
        P(),
        P(None, "tp"),
        P(("grp", "ep"), None),
        P(),
        P(("grp", "ep"), None),
        P(("grp", "ep"), None),
        P("ep", None, "tp"),
        P("ep", None, "tp"),
        P("ep", "tp", None),
        P(),
    )
    out_specs = (P(("grp", "ep"), "tp"), P(("grp", "ep", "tp"), None))
    sizes = (mesh.shape["grp"], mesh.shape["ep"], mesh.shape["tp"])
    return jax.shard_map(
        functools.partial(body, sizes),
        mesh=mesh,
        in_specs=in_specs,
        out_specs=out_specs,
        check_vma=False,
    )
```
